32 devices in a mesh: ep: 8 (over z, y), tp: 4 (over x, core).
Axes of the slice: x: 2, y: 2, z: 4, core: 2. Of those that a mesh axis runs over, the one named last changes fastest.
Arguments:
- conv_value: bfloat16 [3072, 2048], P('ep', 'tp'), may hold values from -36 to 36
- conv_gate: bfloat16 [3072, 2048], P('ep', 'tp'), may hold values from -8 to 8
- conv_taps: bfloat16 [31, 2048], P(None, 'tp'), may hold values from -1 to 1
- conv_gain: float32 [2048], P('tp'), may hold values from 0.1 to 1.9
- conv_proj: bfloat16 [2048, 2048], P('tp'), may hold values from -0.125 to 0.125
- moe_tokens: bfloat16 [3072, 2048], P('ep'), may hold values from -6 to 6
- moe_gain: float32 [2048], replicated, may hold values from 0.1 to 1.9
- routes: int32 [3072, 2], P('ep'), may hold values from 0 to 7, all different within a row; in each aligned block of 384 rows (0 to 383, 384 to 767, ...) at most 144 rows name the same one
- route_weights: float32 [3072, 2], P('ep'), may hold values from 0.3 to 3
- expert_gate: bfloat16 [8, 2048, 1024], P('ep', None, 'tp'), may hold values from -0.125 to 0.125
- expert_up: bfloat16 [8, 2048, 1024], P('ep', None, 'tp'), may hold values from -0.125 to 0.125
- expert_down: bfloat16 [8, 1024, 2048], P('ep', 'tp'), may hold values from -0.1875 to 0.1875
- shared_gate: bfloat16 [2048, 256], replicated, may hold values from -0.125 to 0.125
- shared_up: bfloat16 [2048, 256], replicated, may hold values from -0.125 to 0.125
- shared_down: bfloat16 [256, 2048], P(None, 'tp'), may hold values from -0.375 to 0.375
Outputs:
- conv_result: bfloat16 [3072, 2048], P('ep', 'tp')
- moe_result: bfloat16 [3072, 2048], P('ep', 'tp')
The draws below stay inside these ranges and needn't reach their ends.
Inputs may be any that keep to these rules, and one draw needn't show every extreme that they name: `routes`: each row names 2 different experts. Among the 384 rows of one index of ep (aligned blocks in order) no expert is named more than 144 times, and in some blocks one expert is named exactly 144 times.
All inputs are finite; a program needn't handle non-finite values.
Results may differ from the reference program's by a relative error of at most 0.01.
Values may be sent and summed in bfloat16 or wider, within the bound.
No kernel may reach another device: no remote copies, remote signals or barrier semaphores. Data moves between devices by JAX's collectives and lax.ppermute only.
A program may use at most 64 MiB of HBM per device.

```python
import math
import jax
import jax.numpy as jnp
import numpy as np
from jax import lax

D = 2048
KERNEL = 31
EXPERT_FF = 1024
SHARED_FF = 256
TOPK = 2
TOK_DEV = 384
TOKENS = 3072
EXPERTS = 8
CAPACITY = 144
N_EP = 8
N_TP = 4


def draw_conv_value(key, part):
    first, second = jax.random.split(jax.random.fold_in(key, 11))
    position = jnp.arange(D, dtype=jnp.float32) / (D - 1)
    rough = jnp.exp(jax.random.uniform(second, (D,), jnp.float32, -0.35, 0.35))
    column_scale = jnp.exp(jnp.log(0.5) + position * jnp.log(8.0)) * rough
    values = jnp.clip(jax.random.normal(first, (TOKENS, D), jnp.float32), -6.0, 6.0)
    return (values * column_scale[None, :]).astype(jnp.bfloat16)


def levels(own_key, extent, pieces, low, largest):
    level, own = 1.0, jax.random.fold_in(own_key, 6)
    for dim, blocks in pieces:
        draws = jnp.exp(jax.random.uniform(jax.random.fold_in(own, dim), (blocks,), jnp.float32, low / len(pieces), largest / len(pieces)))
        level = level * jnp.repeat(draws, extent[dim] // blocks).reshape([-1 if axis == dim else 1 for axis in range(len(extent))])
    return level


def shared_out(key, own, number, rows, amount, top, most, lean):
    ranking = jax.random.permutation(key, amount)
    packed, ordinary = portions_of(amount, rows * top, most, lean, True), portions_of(amount, rows * top, most, lean, False)
    places = jnp.arange(amount)

    def named(lengths, turn):
        used = int((lengths > 0).sum())
        fixed = max(1, used // 4)
        shifted = fixed + (places - fixed + turn * (used - fixed)) % max(1, amount - fixed)
        return jnp.zeros((amount,), jnp.int32).at[ranking[jnp.where(places < fixed, places, shifted)]].set(jnp.asarray(lengths, jnp.int32))

    lengths = jnp.where(number % 4 == 0, named(packed, number // 4), named(ordinary, number - number // 4 - 1))
    mixed = jax.random.permutation(jax.random.fold_in(own, 3), amount)
    donor, taker = mixed[0:amount // 2 * 2:2], mixed[1:amount // 2 * 2:2]
    room = jnp.minimum(lengths[donor] - 1, most - lengths[taker]) // 2
    room = jnp.where((donor == ranking[0]) | (taker == ranking[0]) | (lengths[taker] == 0), 0, jnp.maximum(room, 0))
    shifted = jax.random.randint(jax.random.fold_in(own, 4), (amount // 2,), 0, 1 << 20) % (room + 1)
    lengths = lengths.at[donor].add(-shifted).at[taker].add(shifted)
    members = jnp.searchsorted(jnp.cumsum(lengths), jnp.arange(rows * top), side="right").astype(jnp.int32)
    table = members.reshape(top, rows).T
    table = table[jax.random.permutation(jax.random.fold_in(own, 1), rows)]
    turn = jax.random.randint(jax.random.fold_in(own, 2), (rows, 1), 0, top)
    return jnp.take_along_axis(table, (jnp.arange(top)[None, :] + turn) % top, axis=1)


def portions_of(amount, total, reach, skew, full):
    portions = [(1 << 20) // math.isqrt(grade ** skew) + 1 for grade in range(1, amount + 1)]
    largest = reach if full else min(reach, max(-(-total // amount), total * portions[0] // sum(portions)))
    least = 1 if total - largest >= amount - 1 else 0
    given, spare = [largest] + [least] * (amount - 1), total - largest - least * (amount - 1)
    while spare > 0:
        movable = [i for i in range(1, amount) if given[i] < largest] or [i for i in range(1, amount) if given[i] < reach]
        mass, budget = sum([portions[i] for i in movable]), spare
        for i in movable:
            extra = min(reach - given[i], max(1, budget * portions[i] // mass), spare)
            given[i] = given[i] + extra
            spare = spare - extra
    return np.array(given)


def normal_values(stream_key, dims, deviation, limit, shards=(), kind=jnp.bfloat16):
    values = jax.random.normal(stream_key, dims, jnp.float32) * deviation
    if len(shards) > 0:
        values = levels(stream_key, dims, shards, -0.22, 0.18) * values
    return jnp.clip(values, min=-limit, max=limit).astype(kind)


def setup_inputs(seed: int = 0) -> dict:
    streams_of = jax.random.split(jax.random.key(seed), 16)
    conv_value = draw_conv_value(jax.random.fold_in(streams_of[15], 71), 0)
    conv_gate = normal_values(streams_of[1], (TOKENS, D), 1.5, 8.0, ((0, 8), (1, 4)))
    conv_taps = normal_values(streams_of[2], (KERNEL, D), KERNEL ** -0.5, 1.0, ((1, 4),))
    conv_gain = jnp.clip(1.0 + 0.18 * jax.random.normal(streams_of[3], (D,), jnp.float32), 0.1, 1.9)
    conv_proj = normal_values(streams_of[4], (D, D), D ** -0.5, 0.125, ((0, 4),))
    moe_tokens = normal_values(streams_of[5], (TOKENS, D), 1.0, 6.0, ((0, 8),))
    moe_gain = jnp.clip(1.0 + 0.18 * jax.random.normal(streams_of[6], (D,), jnp.float32), 0.1, 1.9)
    routes_keys = jax.random.split(jax.random.fold_in(streams_of[7], 1), TOKENS // TOK_DEV)
    routes_turns = jax.random.permutation(jax.random.fold_in(streams_of[7], 3), TOKENS // TOK_DEV)
    routes = jax.vmap(lambda own, number: shared_out(jax.random.fold_in(streams_of[7], 2), own, number, TOK_DEV, EXPERTS, TOPK, CAPACITY, 1))(routes_keys, routes_turns).reshape((TOKENS, TOPK))
    route_weights = jnp.clip(jnp.exp(math.log(3.0) - 2.3025851 * jax.random.uniform(streams_of[8], (TOKENS, TOPK), jnp.float32) ** levels(streams_of[8], (TOKENS, TOPK), ((0, 8),), -0.2, 0.2)), 0.3, 3.0)
    expert_gate = normal_values(streams_of[9], (EXPERTS, D, EXPERT_FF), D ** -0.5, 0.125, ((0, 8), (2, 4)))
    expert_up = normal_values(streams_of[10], (EXPERTS, D, EXPERT_FF), D ** -0.5, 0.125, ((0, 8), (2, 4)))
    expert_down = normal_values(streams_of[11], (EXPERTS, EXPERT_FF, D), EXPERT_FF ** -0.5, 0.1875, ((0, 8), (1, 4)))
    shared_gate = normal_values(streams_of[12], (D, SHARED_FF), D ** -0.5, 0.125)
    shared_up = normal_values(streams_of[13], (D, SHARED_FF), D ** -0.5, 0.125)
    shared_down = normal_values(streams_of[14], (SHARED_FF, D), SHARED_FF ** -0.5, 0.375, ((1, 4),))
    return {"conv_value": conv_value, "conv_gate": conv_gate, "conv_taps": conv_taps, "conv_gain": conv_gain, "conv_proj": conv_proj, "moe_tokens": moe_tokens, "moe_gain": moe_gain, "routes": routes, "route_weights": route_weights, "expert_gate": expert_gate, "expert_up": expert_up, "expert_down": expert_down, "shared_gate": shared_gate, "shared_up": shared_up, "shared_down": shared_down}


epsilon = 1e-05

def rounded_block(product):
    return lax.optimization_barrier(product.astype(jnp.bfloat16)).astype(jnp.float32)

def reference(conv_value, conv_gate, conv_taps, conv_gain, conv_proj, moe_tokens, moe_gain, routes, route_weights, expert_gate, expert_up, expert_down, shared_gate, shared_up, shared_down):
    gated_rows = (conv_value.astype(jnp.float32) * jax.nn.sigmoid(conv_gate.astype(jnp.float32))).astype(jnp.bfloat16)
    padded = jnp.concatenate([jnp.zeros((KERNEL - 1, D), jnp.bfloat16), gated_rows], axis=0).astype(jnp.float32)
    tap_weights = conv_taps.astype(jnp.float32)
    convolved = jnp.zeros((TOKENS, D), jnp.float32)
    for offset in range(KERNEL):
        convolved = convolved + tap_weights[offset][None, :] * padded[offset:offset + TOKENS]
    average = lax.optimization_barrier(jnp.sum(convolved, axis=1)) / D
    variance = lax.optimization_barrier(jnp.sum(convolved * convolved, axis=1)) / D - average * average
    scaled = (convolved - average[:, None]) * lax.rsqrt(variance + epsilon)[:, None] * conv_gain[None, :]
    activated = jax.nn.silu(scaled).astype(jnp.bfloat16)
    block_width = D // N_TP
    conv_total = jnp.zeros((TOKENS, D), jnp.float32)
    for block in range(N_TP):
        product = jnp.dot(activated[:, block * block_width:(block + 1) * block_width], conv_proj[block * block_width:(block + 1) * block_width], preferred_element_type=jnp.float32)
        conv_total = conv_total + rounded_block(product)
    conv_result = conv_total.astype(jnp.bfloat16)
    tokens = moe_tokens.astype(jnp.float32)
    token_mean = lax.optimization_barrier(jnp.mean(tokens, axis=1, keepdims=True))
    centered = tokens - token_mean
    token_var = lax.optimization_barrier(jnp.mean(centered * centered, axis=1, keepdims=True))
    normalized = (centered * lax.rsqrt(token_var + epsilon) * moe_gain[None, :]).astype(jnp.bfloat16)
    shared_hidden = (jax.nn.silu(jnp.dot(normalized, shared_gate, preferred_element_type=jnp.float32)) * jnp.dot(normalized, shared_up, preferred_element_type=jnp.float32)).astype(jnp.bfloat16)
    shared_part = jnp.dot(shared_hidden, shared_down, preferred_element_type=jnp.float32)
    entries = TOKENS * TOPK
    flat_routes = routes.reshape(-1).astype(jnp.int32)
    flat_index = jnp.arange(entries, dtype=jnp.int32)
    slot_count = N_EP * CAPACITY
    hidden_width = EXPERT_FF // N_TP

    def one_expert(carried, expert):
        chosen = (flat_routes == expert).astype(jnp.int32)
        order = (jnp.cumsum(chosen) - chosen).astype(jnp.int32)
        target = jnp.where(chosen > 0, order, slot_count).astype(jnp.int32)
        source_row = jnp.zeros((slot_count,), jnp.int32).at[target].set(flat_index, mode='drop')
        filled = jnp.zeros((slot_count,), jnp.int32).at[target].set(jnp.ones((entries,), jnp.int32), mode='drop')
        rows_in = normalized[(source_row // TOPK).astype(jnp.int32)]
        hidden = (jax.nn.silu(jnp.dot(rows_in, expert_gate[expert], preferred_element_type=jnp.float32)) * jnp.dot(rows_in, expert_up[expert], preferred_element_type=jnp.float32)).astype(jnp.bfloat16)
        down_rows = expert_down[expert]
        total = jnp.zeros((slot_count, D), jnp.float32)
        for block in range(N_TP):
            product = jnp.dot(hidden[:, block * hidden_width:(block + 1) * hidden_width], down_rows[block * hidden_width:(block + 1) * hidden_width], preferred_element_type=jnp.float32)
            total = total + rounded_block(product)
        write_at = jnp.where(filled > 0, source_row, entries).astype(jnp.int32)
        carried = carried.at[write_at].set(total.astype(jnp.bfloat16), mode='drop')
        return (carried, None)
    expert_rows, _ = lax.scan(one_expert, jnp.zeros((entries, D), jnp.bfloat16), jnp.arange(EXPERTS, dtype=jnp.int32))
    expert_rows = expert_rows.reshape(TOKENS, TOPK, D)
    moe_total = shared_part
    for choice_index in range(TOPK):
        moe_total = moe_total + route_weights[:, choice_index][:, None] * expert_rows[:, choice_index].astype(jnp.float32)
    moe_result = moe_total.astype(jnp.bfloat16)
    return (conv_result, moe_result)
```

```python
import jax
import jax.numpy as jnp
from jax import lax
from jax.sharding import PartitionSpec as P

epsilon = 1e-05


def passed_along(value, axis, by):
    devices = lax.axis_size(axis)
    pairs = [(i, i + by) for i in range(devices) if 0 <= i + by < devices]
    return lax.ppermute(value, axis, pairs)


def tp_swap(value, by):
    devices = lax.axis_size("tp")
    return lax.ppermute(value, "tp", [(t, t ^ by) for t in range(devices)])


def ep_swap(value, pair):
    n_ep, n_tp = lax.axis_size("ep"), lax.axis_size("tp")
    pairs = [
        (i * n_tp + t, (i ^ (2 * pair + (t & 1))) * n_tp + t)
        for i in range(n_ep)
        for t in range(n_tp)
    ]
    return lax.ppermute(value, ("ep", "tp"), pairs)


def dot32(a, b):
    return jnp.dot(a, b, preferred_element_type=jnp.float32)


def swiglu(rows, gate, up):
    return (jax.nn.silu(dot32(rows, gate)) * dot32(rows, up)).astype(jnp.bfloat16)


def conv_half(conv_value, conv_gate, conv_taps, conv_gain, conv_proj, model_width):
    tok_rows = conv_value.shape[0]
    kernel = conv_taps.shape[0]
    gated_rows = (
        conv_value.astype(jnp.float32) * jax.nn.sigmoid(conv_gate.astype(jnp.float32))
    ).astype(jnp.bfloat16)
    previous = passed_along(gated_rows[tok_rows - (kernel - 1) :], "ep", 1)
    padded = jnp.concatenate([previous, gated_rows], axis=0).astype(jnp.float32)
    tap_weights = conv_taps.astype(jnp.float32)
    convolved = jnp.zeros(gated_rows.shape, jnp.float32)
    for offset in range(kernel):
        convolved = convolved + tap_weights[offset][None, :] * padded[offset : offset + tok_rows]
    sums = jnp.stack([jnp.sum(convolved, axis=1), jnp.sum(convolved * convolved, axis=1)])
    sums = sums + tp_swap(sums, 1)
    sums = sums + tp_swap(sums, 2)
    average = sums[0] / model_width
    variance = sums[1] / model_width - average * average
    scaled = (
        (convolved - average[:, None]) * lax.rsqrt(variance + epsilon)[:, None] * conv_gain[None, :]
    )
    activated = jax.nn.silu(scaled).astype(jnp.bfloat16)
    t = lax.axis_index("tp")
    width = model_width // lax.axis_size("tp")
    blocks = [
        dot32(activated, lax.dynamic_slice_in_dim(conv_proj, (t ^ by) * width, width, 1))
        for by in range(4)
    ]
    sent = jnp.concatenate([blocks[1], blocks[3]], axis=1).astype(jnp.bfloat16)
    got = tp_swap(sent, 1).astype(jnp.float32)
    keep = blocks[0] + got[:, :width]
    send = (blocks[2] + got[:, width:]).astype(jnp.bfloat16)
    return (keep + tp_swap(send, 2).astype(jnp.float32)).astype(jnp.bfloat16)


def moe_wide(
    normalized, routes, route_weights, expert_gate, expert_up, expert_down, capacity
):
    tok_rows, model_width = normalized.shape
    experts = lax.axis_size("ep")
    top_count = routes.shape[1]
    quarter = model_width // lax.axis_size("tp")
    every = jnp.arange(experts, dtype=jnp.int32)[:, None]
    hit = [routes.T[k][None, :] == every for k in range(top_count)]
    place, weight = slots_of(hit, route_weights, capacity)
    columns = lax.dynamic_slice_in_dim(normalized, lax.axis_index("tp") * quarter, quarter, 1)
    slots = experts * capacity
    outgoing = dot32(place.astype(jnp.bfloat16).reshape(slots, tok_rows), columns)
    outgoing = outgoing.astype(jnp.bfloat16).reshape(experts, capacity, quarter)
    arrived = lax.all_to_all(outgoing, "ep", split_axis=0, concat_axis=0, tiled=True)
    arrived = lax.all_gather(arrived, "tp", axis=2, tiled=True)
    hidden = swiglu(arrived.reshape(slots, model_width), expert_gate, expert_up)
    partial = dot32(hidden, expert_down).astype(jnp.bfloat16)
    rows = lax.psum_scatter(partial, "tp", scatter_dimension=1, tiled=True)
    rows = rows.reshape(experts, capacity, quarter)
    returned = lax.all_to_all(rows, "ep", split_axis=0, concat_axis=0, tiled=True)
    out = jnp.where(place, weight[:, None, :], 0.0).astype(jnp.bfloat16)
    return lax.dot_general(
        out.reshape(slots, tok_rows), returned.reshape(slots, quarter), (((0,), (0,)), ((), ())),
        preferred_element_type=jnp.float32,
    )


def slots_of(hit, route_weights, capacity):
    tok_rows = route_weights.shape[0]
    chosen = hit[0]
    for one in hit[1:]:
        chosen = chosen | one
    order = jnp.arange(tok_rows, dtype=jnp.int32)
    earlier = (order[:, None] < order[None, :]).astype(jnp.bfloat16)
    rank = dot32(chosen.astype(jnp.bfloat16), earlier).astype(jnp.int32)
    slot = jnp.where(chosen, rank, -1)
    place = slot[:, None, :] == jnp.arange(capacity, dtype=jnp.int32)[None, :, None]
    weight = sum(
        jnp.where(one, route_weights.T[k][None, :], 0.0) for k, one in enumerate(hit)
    )
    return place, weight


def local(
    conv_value,
    conv_gate,
    conv_taps,
    conv_gain,
    conv_proj,
    moe_tokens,
    moe_gain,
    routes,
    route_weights,
    expert_gate,
    expert_up,
    expert_down,
    shared_gate,
    shared_up,
    shared_down,
):
    model_width = moe_tokens.shape[1]
    half = model_width // 2
    quarter = model_width // lax.axis_size("tp")
    tok_rows = moe_tokens.shape[0]
    experts = lax.axis_size("ep")
    top_count = routes.shape[1]
    capacity = 3 * tok_rows * top_count // (2 * experts)
    n_pairs = experts // 2
    i, t = lax.axis_index("ep"), lax.axis_index("tp")
    side, parity = t >> 1, t & 1

    tokens = moe_tokens.astype(jnp.float32)
    token_mean = jnp.mean(tokens, axis=1, keepdims=True)
    centered = tokens - token_mean
    token_var = jnp.mean(centered * centered, axis=1, keepdims=True)
    normalized = (centered * lax.rsqrt(token_var + epsilon) * moe_gain[None, :]).astype(
        jnp.bfloat16
    )

    if experts > 8:
        conv_result = conv_half(
            conv_value, conv_gate, conv_taps, conv_gain, conv_proj, model_width
        )
        shared_part = dot32(swiglu(normalized, shared_gate, shared_up), shared_down)
        routed = moe_wide(
            normalized, routes, route_weights, expert_gate[0], expert_up[0], expert_down[0], capacity
        )
        return (conv_result, (shared_part + routed).astype(jnp.bfloat16))

    down = expert_down[0]
    mine_down = lax.dynamic_slice_in_dim(down, side * half, half, 1)
    far_down = tp_swap(lax.dynamic_slice_in_dim(down, (1 - side) * half, half, 1), 2)
    pair_down = tp_swap(jnp.concatenate([mine_down, far_down], axis=0), 1)
    width = down.shape[0]
    down_a = jnp.concatenate([mine_down, pair_down[:width]], axis=0)
    down_b = jnp.concatenate([far_down, pair_down[width:]], axis=0)

    relative = routes.T ^ i ^ parity
    wanted = 2 * jnp.arange(n_pairs, dtype=jnp.int32)[:, None]
    hit = [relative[k][None, :] == wanted for k in range(top_count)]
    place, weight = slots_of(hit, route_weights, capacity)
    place_in = place.astype(jnp.bfloat16)
    place_out = jnp.where(place, weight[:, None, :], 0.0).astype(jnp.bfloat16)

    near = n_pairs // 2
    split = near + (n_pairs - near) // 2
    chunks = [range(near, split), range(split, n_pairs), range(0, near)]
    rows_half = lax.dynamic_slice_in_dim(normalized, side * half, half, 1)
    arrived = {}
    for chunk in chunks:
        for p in chunk:
            rows = dot32(place_in[p], rows_half if p >= near else normalized).astype(jnp.bfloat16)
            arrived[p] = ep_swap(rows, p)

    conv_result = conv_half(
        conv_value, conv_gate, conv_taps, conv_gain, conv_proj, model_width
    )
    shared_hidden = swiglu(normalized, shared_gate, shared_up)
    shared_part = dot32(shared_hidden, shared_down)

    gate = expert_gate[0]
    up = expert_up[0]
    returned = {}
    for chunk in chunks:
        rows = jnp.concatenate([arrived[p] for p in chunk], axis=0)
        if chunk[0] >= near:
            other = tp_swap(rows, 2)
            low = jnp.where(side == 0, rows, other)
            high = jnp.where(side == 0, other, rows)
            rows = jnp.concatenate([low, high], axis=1)
        theirs = tp_swap(rows, 1)
        hidden = swiglu(jnp.concatenate([theirs, rows], axis=0), gate, up)
        count = rows.shape[0]
        pair_hidden = jnp.concatenate([hidden[count:], tp_swap(hidden[:count], 1)], axis=1)
        far_hidden = tp_swap(pair_hidden, 2)
        out = (dot32(pair_hidden, down_a) + dot32(far_hidden, down_b)).astype(jnp.bfloat16)
        for n, p in enumerate(chunk):
            returned[p] = ep_swap(out[n * capacity : (n + 1) * capacity], p)

    total = jnp.zeros((tok_rows, half), jnp.float32)
    for chunk in chunks:
        for p in chunk:
            total = total + lax.dot_general(
                place_out[p], returned[p], (((0,), (0,)), ((), ())),
                preferred_element_type=jnp.float32,
            )
    keep = lax.dynamic_slice_in_dim(total, parity * quarter, quarter, 1)
    send = lax.dynamic_slice_in_dim(total, (1 - parity) * quarter, quarter, 1)
    moe_result = (
        shared_part + keep + tp_swap(send.astype(jnp.bfloat16), 1).astype(jnp.float32)
    ).astype(jnp.bfloat16)
    return (conv_result, moe_result)


def solution(mesh):
    placed = (
        P("ep", "tp"),
        P("ep", "tp"),
        P(None, "tp"),
        P("tp"),
        P("tp", None),
        P("ep", None),
        P(),
        P("ep", None),
        P("ep", None),
        P("ep", None, "tp"),
        P("ep", None, "tp"),
        P("ep", "tp", None),
        P(),
        P(),
        P(None, "tp"),
    )
    return jax.shard_map(
        local, mesh=mesh, in_specs=placed, out_specs=(P("ep", "tp"), P("ep", "tp")), check_vma=False
    )
```

```python
import functools

import jax
import jax.numpy as jnp
from jax import lax
from jax.experimental import pallas as pl
from jax.experimental.pallas import tpu as pltpu
from jax.sharding import PartitionSpec as P


epsilon = 1e-05


def passed_along(value, axis, by):
    devices = lax.axis_size(axis)
    pairs = [(i, i + by) for i in range(devices) if 0 <= i + by < devices]
    return lax.ppermute(value, axis, pairs)


def tp_swap(value, by):
    devices = lax.axis_size("tp")
    return lax.ppermute(value, "tp", [(t, t ^ by) for t in range(devices)])


def ep_swap(value, pair):
    n_ep, n_tp = lax.axis_size("ep"), lax.axis_size("tp")
    pairs = [
        (i * n_tp + t, (i ^ (2 * pair + (t & 1))) * n_tp + t)
        for i in range(n_ep)
        for t in range(n_tp)
    ]
    return lax.ppermute(value, ("ep", "tp"), pairs)


def ep_next(value):
    devices = lax.axis_size("ep")
    return lax.ppermute(value, "ep", [(i, i ^ 1) for i in range(devices)])


def dot32(a, b):
    return jnp.dot(a, b, preferred_element_type=jnp.float32)


def swiglu(rows, gate, up):
    return (jax.nn.silu(dot32(rows, gate)) * dot32(rows, up)).astype(jnp.bfloat16)


def kernel_call(body, outs, *arrays, mib, outside=0, scratch=()):
    arrays = [
        pltpu.with_memory_space_constraint(one, pltpu.HBM) if n < outside else one
        for n, one in enumerate(arrays)
    ]
    return pl.pallas_call(
        body,
        out_shape=[jax.ShapeDtypeStruct(shape, kind) for shape, kind in outs],
        in_specs=[pl.BlockSpec(memory_space=pltpu.HBM)] * outside
        + [pl.BlockSpec(memory_space=pltpu.VMEM)] * (len(arrays) - outside),
        out_specs=[pl.BlockSpec(memory_space=pltpu.VMEM)] * len(outs),
        scratch_shapes=scratch,
        compiler_params=pltpu.CompilerParams(vmem_limit_bytes=mib << 20),
    )(*arrays)


def half_at(which, half):
    return pl.ds(pl.multiple_of(which * half, half), half)


def one_hot(slot, row, count):
    shape = (count, slot.shape[1])
    return slot[row : row + 1, :] == lax.broadcasted_iota(jnp.int32, shape, 0)


def as_bf16(mask):
    return jnp.where(mask, 1.0, 0.0).astype(jnp.bfloat16)


def distances(parity, shape):
    row = lax.broadcasted_iota(jnp.int32, shape, 0)
    return jnp.where(row < 2, row, 2 * (row - 1) + parity)


def gating(value, gate):
    return (value.astype(jnp.float32) * jax.nn.sigmoid(gate.astype(jnp.float32))).astype(
        jnp.bfloat16
    )


def prep_kernel(
    tokens_ref, gain_ref, routes_ref, value_ref, gate_ref, down_ref, norm_ref, slot_ref, last_ref,
    mine_down_ref, other_down_ref, *refs, first_far,
):
    *far_refs, held_ref, held_gain_ref, held_routes_ref, last_value_ref, last_gate_ref, sems = refs
    tok_rows, model_width = tokens_ref.shape
    half = model_width // 2
    i, t = lax.axis_index("ep"), lax.axis_index("tp")
    side, parity = t >> 1, t & 1
    last = pl.ds(value_ref.shape[0] - last_ref.shape[0], last_ref.shape[0])
    parts = 4
    step = tok_rows // parts
    copies = [
        pltpu.make_async_copy(src, dst, sems.at[n])
        for n, (src, dst) in enumerate(
            [(gain_ref, held_gain_ref)]
            + [
                (tokens_ref.at[pl.ds(k * step, step), :], held_ref.at[pl.ds(k * step, step), :])
                for k in range(parts)
            ]
            + [
                (routes_ref, held_routes_ref),
                (down_ref.at[:, half_at(1 - side, half)], other_down_ref),
                (value_ref.at[last, :], last_value_ref),
                (gate_ref.at[last, :], last_gate_ref),
                (down_ref.at[:, half_at(side, half)], mine_down_ref),
            ]
        )
    ]
    for copy in copies:
        copy.start()
    gain_copy, *token_copies = copies[: parts + 1]
    gain_copy.wait()
    block = 16
    for k, copy in enumerate(token_copies):
        copy.wait()

        def rows(n, _):
            at = pl.ds(pl.multiple_of(k * step + n * block, block), block)
            x = held_ref[at, :].astype(jnp.float32)
            centered = x - jnp.mean(x, axis=1, keepdims=True)
            var = jnp.mean(centered * centered, axis=1, keepdims=True)
            norm_ref[at, :] = (centered * lax.rsqrt(var + epsilon) * held_gain_ref[...]).astype(
                jnp.bfloat16
            )
            return 0

        lax.fori_loop(0, step // block, rows, 0, unroll=True)
    for copy in copies[parts + 1 :]:
        copy.wait()
    relative = held_routes_ref[...] ^ i
    table = slot_ref.shape
    wanted = distances(parity, table)
    chosen = relative[0:1, :] == wanted
    for k in range(1, relative.shape[0]):
        chosen = chosen | (relative[k : k + 1, :] == wanted)
    square = (tok_rows, tok_rows)
    earlier = as_bf16(
        lax.broadcasted_iota(jnp.int32, square, 0) < lax.broadcasted_iota(jnp.int32, square, 1)
    )
    rank = dot32(as_bf16(chosen), earlier).astype(jnp.int32)
    capacity = far_refs[0].shape[0]
    turned = rank - parity * (capacity // 2)
    turned = jnp.where(turned < 0, turned + capacity, turned)
    row = lax.broadcasted_iota(jnp.int32, table, 0)
    slot = jnp.where(chosen, jnp.where(row < 2, turned, rank), -1)
    slot_ref[...] = slot
    columns = norm_ref[:, half_at(side, half)]
    for n, ref in enumerate(far_refs):
        ref[...] = dot32(as_bf16(one_hot(slot, first_far + n, ref.shape[0])), columns).astype(
            jnp.bfloat16
        )
    last_ref[...] = gating(last_value_ref[...], last_gate_ref[...])


def conv_kernel(value_ref, gate_ref, before_ref, taps_ref, out_ref, sums_ref, held_ref, total_ref):
    tok_rows, width = value_ref.shape
    kernel, ahead = taps_ref.shape[0], before_ref.shape[0]
    lanes, step = 128, tok_rows // 6
    held_ref[:ahead, :] = before_ref[...].astype(jnp.float32)

    def gate(n, _):
        at = pl.ds(pl.multiple_of(n * 16, 16), 16)
        held_ref[pl.ds(pl.multiple_of(ahead + n * 16, 16), 16), :] = gating(
            value_ref[at, :], gate_ref[at, :]
        ).astype(jnp.float32)
        return 0

    lax.fori_loop(0, tok_rows // 16, gate, 0, unroll=4)
    taps = taps_ref[...].astype(jnp.float32)

    def rows(n, _):
        start = n * step
        ones = squares = jnp.zeros((step, lanes), jnp.float32)
        for lane in range(0, width, lanes):
            x = held_ref[pl.ds(pl.multiple_of(start, 8), step + ahead), lane : lane + lanes]
            x = jnp.concatenate([x, jnp.zeros((8, lanes), jnp.float32)], axis=0)
            out = jnp.zeros((step, lanes), jnp.float32)
            for shift in range(8):
                part = None
                for offset in range(kernel):
                    reach = offset + ahead - (kernel - 1)
                    if reach % 8 != shift:
                        continue
                    low = reach - shift
                    one = taps[offset : offset + 1, lane : lane + lanes] * x[low : low + step + 8]
                    part = one if part is None else part + one
                if part is not None:
                    out = out + part[shift : shift + step]
            out_ref[pl.ds(pl.multiple_of(start, 8), step), lane : lane + lanes] = out
            ones = ones + out
            squares = squares + out * out
        at = pl.ds(pl.multiple_of(start, 8), step)
        total_ref[0, at, :] = ones
        total_ref[1, at, :] = squares
        return 0

    lax.fori_loop(0, tok_rows // step, rows, 0)
    one_row = jnp.ones((8, lanes), jnp.float32)
    first, second = [
        lax.dot_general(
            one_row, total_ref[n], (((1,), (1,)), ((), ())), preferred_element_type=jnp.float32,
            precision=lax.Precision.HIGHEST,
        )
        for n in range(2)
    ]
    row = lax.broadcasted_iota(jnp.int32, first.shape, 0)
    sums_ref[...] = jnp.where(row == 0, first, second)


def act_kernel(
    conv_ref, sums_ref, more_ref, gain_ref, proj_ref, sent_ref, keep_ref, far_ref, act_ref,
    mean_ref, scale_ref,
):
    tok_rows, width = conv_ref.shape
    model_width = proj_ref.shape[1]
    lanes = 128
    sums = sums_ref[...] + more_ref[...]
    row = lax.broadcasted_iota(jnp.int32, (sums.shape[0], lanes), 0)
    average, square = [
        lax.dot_general(
            sums, jnp.where(row == n, 1.0, 0.0), (((0,), (0,)), ((), ())),
            preferred_element_type=jnp.float32, precision=lax.Precision.HIGHEST,
        )
        / model_width
        for n in range(2)
    ]
    mean_ref[...] = average
    scale_ref[...] = lax.rsqrt(square - average * average + epsilon)

    def rows(n, _):
        at = pl.ds(pl.multiple_of(n * 16, 16), 16)
        mean, scale = mean_ref[at, :], scale_ref[at, :]
        for lane in range(0, width, lanes):
            cols = slice(lane, lane + lanes)
            scaled = (conv_ref[at, cols] - mean) * scale * gain_ref[:, cols]
            act_ref[at, cols] = jax.nn.silu(scaled).astype(jnp.bfloat16)
        return 0

    lax.fori_loop(0, tok_rows // 16, rows, 0, unroll=4)
    t = lax.axis_index("tp")
    act = act_ref[...]

    def product(by):
        return dot32(act, proj_ref[:, half_at(t ^ by, width)])

    sent_ref[:, :width] = product(1).astype(jnp.bfloat16)
    sent_ref[:, width:] = product(3).astype(jnp.bfloat16)
    keep_ref[...] = product(0)
    far_ref[...] = product(2)


def crone_kernel(keep_ref, far_ref, got_ref, more_ref, send_ref):
    width = keep_ref.shape[1]
    more_ref[...] = keep_ref[...] + got_ref[:, :width].astype(jnp.float32)
    send_ref[...] = (far_ref[...] + got_ref[:, width:].astype(jnp.float32)).astype(jnp.bfloat16)


def add_kernel(a_ref, b_ref, out_ref):
    out_ref[...] = (a_ref[...] + b_ref[...].astype(jnp.float32)).astype(jnp.bfloat16)


def down_kernel(mine_ref, other_ref, d0_ref, d1_ref, d2_ref, d3_ref, *out_refs):
    width = d0_ref.shape[0]
    at = 0
    for out in out_refs:
        rows = slice(at, at + out.shape[0])
        at += out.shape[0]
        out[...] = (
            dot32(mine_ref[rows, :width], d0_ref[...])
            + dot32(mine_ref[rows, width:], d1_ref[...])
            + dot32(other_ref[rows, :width], d2_ref[...])
            + dot32(other_ref[rows, width:], d3_ref[...])
        ).astype(jnp.bfloat16)


def pick_kernel(slot_ref, routes_ref, weights_ref, keep_ref, *refs, which):
    refs = list(refs)
    sent_ref = None if which[0] == 0 else refs.pop(0)
    *back, keep_out, send_out = refs
    i, t = lax.axis_index("ep"), lax.axis_index("tp")
    parity = t & 1
    quarter = keep_out.shape[1]
    relative = routes_ref[...] ^ i
    slot = slot_ref[...]
    wanted = distances(parity, slot.shape)
    weight = jnp.zeros(slot.shape, jnp.float32)
    for k in range(relative.shape[0]):
        weight = weight + jnp.where(relative[k : k + 1, :] == wanted, weights_ref[k : k + 1, :], 0.0)
    places = [
        jnp.where(one_hot(slot, row, ref.shape[0]), weight[row : row + 1, :], 0.0).astype(jnp.bfloat16)
        for row, ref in zip(which, back)
    ]

    def total(start, at):
        for place, ref in zip(places, back):
            part = lax.dot_general(
                place, ref[:, half_at(at, quarter)], (((0,), (0,)), ((), ())),
                preferred_element_type=jnp.float32,
            )
            start = part if start is None else start + part
        return start

    send = total(None if sent_ref is None else sent_ref[...], 1 - parity)
    send_out[...] = send.astype(send_out.dtype)
    keep_out[...] = total(keep_ref[...], parity)


def near_kernel(norm_ref, slot_ref, *near_refs):
    slot = slot_ref[...]
    for n, ref in reversed(list(enumerate(near_refs))):
        ref[...] = dot32(as_bf16(one_hot(slot, n, ref.shape[0])), norm_ref[...]).astype(jnp.bfloat16)


def far_expert_kernel(a_ref, b_ref, gate_ref, up_ref, gate2_ref, up2_ref, out_ref):
    half, width = gate_ref.shape[0] // 2, gate_ref.shape[1]
    side = lax.axis_index("tp") >> 1
    here, there = half_at(side, half), half_at(1 - side, half)
    a, b = a_ref[...], b_ref[...]
    for at, gates, ups in ((0, gate_ref, up_ref), (width, gate2_ref, up2_ref)):
        gate = dot32(a, gates[here, :]) + dot32(b, gates[there, :])
        up = dot32(a, ups[here, :]) + dot32(b, ups[there, :])
        out_ref[:, at : at + width] = (jax.nn.silu(gate) * up).astype(jnp.bfloat16)


def near_expert_kernel(*refs):
    *rows, gate_ref, up_ref, gate2_ref, up2_ref, out_ref = refs
    width = gate_ref.shape[1]
    low = 0
    for ref in rows:
        high = low + ref.shape[0]
        for at, gates, ups in ((0, gate_ref, up_ref), (width, gate2_ref, up2_ref)):
            out_ref[low:high, at : at + width] = swiglu(ref[...], gates[...], ups[...])
        low = high


def shared_kernel(norm_ref, gate_ref, up_ref, down_ref, out_ref):
    norm = norm_ref[...]
    hidden = jax.nn.silu(dot32(norm, gate_ref[...])) * dot32(norm, up_ref[...])
    out_ref[...] = dot32(hidden.astype(jnp.bfloat16), down_ref[...])


def conv_half(
    conv_value, conv_gate, last, conv_taps, conv_gain, conv_proj, model_width
):
    tok_rows = conv_value.shape[0]
    kernel = conv_taps.shape[0]
    gated_rows = gating(conv_value, conv_gate)
    previous = passed_along(last, "ep", 1)
    padded = jnp.concatenate([previous[last.shape[0] - (kernel - 1) :], gated_rows], axis=0)
    padded = padded.astype(jnp.float32)
    tap_weights = conv_taps.astype(jnp.float32)
    convolved = jnp.zeros(gated_rows.shape, jnp.float32)
    for offset in range(kernel):
        convolved = convolved + tap_weights[offset][None, :] * padded[offset : offset + tok_rows]
    sums = jnp.stack([jnp.sum(convolved, axis=1), jnp.sum(convolved * convolved, axis=1)])
    sums = sums + tp_swap(sums, 1)
    sums = sums + tp_swap(sums, 2)
    average = sums[0] / model_width
    variance = sums[1] / model_width - average * average
    scaled = (
        (convolved - average[:, None]) * lax.rsqrt(variance + epsilon)[:, None] * conv_gain[None, :]
    )
    activated = jax.nn.silu(scaled).astype(jnp.bfloat16)
    t = lax.axis_index("tp")
    width = model_width // lax.axis_size("tp")
    keep, send, keep_far, send_far = [
        dot32(activated, lax.dynamic_slice_in_dim(conv_proj, (t ^ by) * width, width, 1))
        for by in range(4)
    ]
    got = tp_swap(jnp.concatenate([send, send_far], axis=1).astype(jnp.bfloat16), 1)
    keep = keep + got[:, :width].astype(jnp.float32)
    far = (keep_far + got[:, width:].astype(jnp.float32)).astype(jnp.bfloat16)
    return (keep + tp_swap(far, 2).astype(jnp.float32)).astype(jnp.bfloat16)


def conv_paired(conv_value, conv_gate, last, conv_taps, conv_gain, conv_proj):
    bf16, f32 = jnp.bfloat16, jnp.float32
    tok_rows, width = conv_value.shape
    before = passed_along(last, "ep", 1)
    lanes, table = (tok_rows, 128), (8, tok_rows)
    block, wide_block = (tok_rows, width), (tok_rows, 2 * width)
    convolved, sums = kernel_call(
        conv_kernel, [(block, f32), (table, f32)], conv_value, conv_gate, before, conv_taps,
        mib=6,
        scratch=[
            pltpu.VMEM((tok_rows + last.shape[0], width), f32), pltpu.VMEM((2, *lanes), f32)
        ],
    )
    sums = sums + tp_swap(sums, 1)
    sent, keep, far = kernel_call(
        act_kernel, [(wide_block, bf16), (block, f32), (block, f32)], convolved, sums,
        tp_swap(sums, 2), conv_gain[None, :], conv_proj, mib=8,
        scratch=[pltpu.VMEM(block, bf16), pltpu.VMEM(lanes, f32), pltpu.VMEM(lanes, f32)],
    )
    keep, far = kernel_call(
        crone_kernel, [(block, f32), (block, bf16)], keep, far, tp_swap(sent, 1),
        mib=6,
    )
    return kernel_call(add_kernel, [(block, bf16)], keep, tp_swap(far, 2), mib=4)[0]


def moe_wide(
    normalized, routes, route_weights, expert_gate, expert_up, expert_down, capacity
):
    tok_rows, model_width = normalized.shape
    experts = lax.axis_size("ep")
    top_count = routes.shape[1]
    quarter = model_width // lax.axis_size("tp")
    every = jnp.arange(experts, dtype=jnp.int32)[:, None]
    hit = [routes.T[k][None, :] == every for k in range(top_count)]
    place, weight = slots_of(hit, route_weights, capacity)
    columns = lax.dynamic_slice_in_dim(normalized, lax.axis_index("tp") * quarter, quarter, 1)
    slots = experts * capacity
    outgoing = dot32(place.astype(jnp.bfloat16).reshape(slots, tok_rows), columns)
    outgoing = outgoing.astype(jnp.bfloat16).reshape(experts, capacity, quarter)
    arrived = lax.all_to_all(outgoing, "ep", split_axis=0, concat_axis=0, tiled=True)
    arrived = lax.all_gather(arrived, "tp", axis=2, tiled=True)
    hidden = swiglu(arrived.reshape(slots, model_width), expert_gate, expert_up)
    partial = dot32(hidden, expert_down).astype(jnp.bfloat16)
    rows = lax.psum_scatter(partial, "tp", scatter_dimension=1, tiled=True)
    rows = rows.reshape(experts, capacity, quarter)
    returned = lax.all_to_all(rows, "ep", split_axis=0, concat_axis=0, tiled=True)
    out = jnp.where(place, weight[:, None, :], 0.0).astype(jnp.bfloat16)
    return lax.dot_general(
        out.reshape(slots, tok_rows), returned.reshape(slots, quarter), (((0,), (0,)), ((), ())),
        preferred_element_type=jnp.float32,
    )


def slots_of(hit, route_weights, capacity):
    tok_rows = route_weights.shape[0]
    chosen = hit[0]
    for one in hit[1:]:
        chosen = chosen | one
    order = jnp.arange(tok_rows, dtype=jnp.int32)
    earlier = (order[:, None] < order[None, :]).astype(jnp.bfloat16)
    rank = dot32(chosen.astype(jnp.bfloat16), earlier).astype(jnp.int32)
    slot = jnp.where(chosen, rank, -1)
    place = slot[:, None, :] == jnp.arange(capacity, dtype=jnp.int32)[None, :, None]
    weight = sum(
        jnp.where(one, route_weights.T[k][None, :], 0.0) for k, one in enumerate(hit)
    )
    return place, weight


def local(
    conv_value,
    conv_gate,
    conv_taps,
    conv_gain,
    conv_proj,
    moe_tokens,
    moe_gain,
    routes,
    route_weights,
    expert_gate,
    expert_up,
    expert_down,
    shared_gate,
    shared_up,
    shared_down,
):
    tok_rows = moe_tokens.shape[0]
    experts = lax.axis_size("ep")
    capacity = 3 * tok_rows * routes.shape[1] // (2 * experts)
    if experts != 8:
        return wide(
            conv_value, conv_gate, conv_taps, conv_gain, conv_proj, moe_tokens, moe_gain, routes,
            route_weights, expert_gate, expert_up, expert_down, shared_gate, shared_up, shared_down,
            capacity,
        )
    return paired(
        conv_value, conv_gate, conv_taps, conv_gain, conv_proj, moe_tokens, moe_gain, routes,
        route_weights, expert_gate, expert_up, expert_down, shared_gate, shared_up, shared_down,
        capacity,
    )


def paired(
    conv_value, conv_gate, conv_taps, conv_gain, conv_proj, moe_tokens, moe_gain, routes,
    route_weights, expert_gate, expert_up, expert_down, shared_gate, shared_up, shared_down, capacity,
):
    bf16, f32 = jnp.bfloat16, jnp.float32
    tok_rows, model_width = moe_tokens.shape
    half = model_width // 2
    quarter = model_width // lax.axis_size("tp")
    n_pairs = lax.axis_size("ep") // 2
    near = n_pairs // 2
    routes_t, weights_t = routes.T, route_weights.T
    far = range(near, n_pairs)
    some = capacity // 2

    table = (n_pairs + 1, tok_rows)
    last = (-(-(conv_taps.shape[0] - 1) // 16) * 16, quarter)
    down = expert_down[0]
    width = down.shape[0]
    norm, slot, last_rows, d0, other_down, *messages = kernel_call(
        functools.partial(prep_kernel, first_far=near + 1),
        [((tok_rows, model_width), bf16), (table, jnp.int32), (last, bf16)]
        + [((width, half), bf16)] * 2 + [((capacity, half), bf16)] * len(far),
        moe_tokens, moe_gain[None, :], routes_t, conv_value, conv_gate, down, mib=16,
        outside=6,
        scratch=[
            pltpu.VMEM((tok_rows, model_width), bf16), pltpu.VMEM((1, model_width), f32),
            pltpu.VMEM(routes_t.shape, jnp.int32), pltpu.VMEM(last, bf16), pltpu.VMEM(last, bf16),
            pltpu.SemaphoreType.DMA((10,)),
        ],
    )
    arrived = {p: ep_swap(messages[p - near], p) for p in far}
    own, *messages = kernel_call(
        near_kernel,
        [((some, model_width), bf16)] * 2 + [((capacity, model_width), bf16)] * (near - 1),
        norm, slot, mib=8,
    )
    for p in range(1, near):
        arrived[p] = ep_swap(messages[p], p)
    arrived[0] = ep_next(messages[0])

    d2 = tp_swap(other_down, 2)
    downs = (d0, tp_swap(d0, 1), d2, tp_swap(d2, 1))

    conv_result = conv_paired(conv_value, conv_gate, last_rows, conv_taps, conv_gain, conv_proj)
    (keep,) = kernel_call(
        shared_kernel, [((tok_rows, quarter), f32)], norm, shared_gate, shared_up,
        shared_down, mib=8,
    )

    gate, up = expert_gate[0], expert_up[0]
    weights = (gate, up, tp_swap(gate, 1), tp_swap(up, 1))
    returned = {}

    def completed(hidden, sizes):
        return kernel_call(
            down_kernel, [((size, half), bf16) for size in sizes], hidden,
            tp_swap(hidden, 2), *downs, mib=6,
        )

    for p in far:
        (hidden,) = kernel_call(
            far_expert_kernel, [((capacity, 2 * width), bf16)], arrived[p],
            tp_swap(arrived[p], 2), *weights, mib=4,
        )
        returned[p] = ep_swap(completed(hidden, [capacity])[0], p)
    (hidden,) = kernel_call(
        near_expert_kernel, [((capacity, 2 * width), bf16)], own, arrived[0], *weights,
        mib=6,
    )
    here, beside = completed(hidden, [some, some])
    for p in range(1, near):
        (hidden,) = kernel_call(
            near_expert_kernel, [((capacity, 2 * width), bf16)], arrived[p], *weights,
            mib=6,
        )
        returned[p] = ep_swap(completed(hidden, [capacity])[0], p)
    back = [here, ep_next(beside)] + [returned[p] for p in range(1, n_pairs)]

    table = (slot, routes_t, weights_t)
    early = n_pairs
    keep, sent = kernel_call(
        functools.partial(pick_kernel, which=tuple(range(early))),
        [((tok_rows, quarter), f32)] * 2, *table, keep, *back[:early], mib=6,
    )
    keep, sent = kernel_call(
        functools.partial(pick_kernel, which=tuple(range(early, len(back)))),
        [((tok_rows, quarter), f32), ((tok_rows, quarter), bf16)], *table, keep, sent,
        *back[early:], mib=6,
    )
    (moe_result,) = kernel_call(
        add_kernel, [((tok_rows, quarter), bf16)], keep, tp_swap(sent, 1), mib=4
    )
    return (conv_result, moe_result)


def wide(
    conv_value, conv_gate, conv_taps, conv_gain, conv_proj, moe_tokens, moe_gain, routes,
    route_weights, expert_gate, expert_up, expert_down, shared_gate, shared_up, shared_down, capacity,
):
    model_width = moe_tokens.shape[1]
    tokens = moe_tokens.astype(jnp.float32)
    token_mean = jnp.mean(tokens, axis=1, keepdims=True)
    centered = tokens - token_mean
    token_var = jnp.mean(centered * centered, axis=1, keepdims=True)
    normalized = (centered * lax.rsqrt(token_var + epsilon) * moe_gain[None, :]).astype(
        jnp.bfloat16
    )

    reach = conv_value.shape[0] - (conv_taps.shape[0] - 1)
    conv_result = conv_half(
        conv_value, conv_gate, gating(conv_value[reach:], conv_gate[reach:]), conv_taps, conv_gain,
        conv_proj, model_width,
    )
    shared_part = dot32(swiglu(normalized, shared_gate, shared_up), shared_down)
    routed = moe_wide(
        normalized, routes, route_weights, expert_gate[0], expert_up[0], expert_down[0], capacity
    )
    return (conv_result, (shared_part + routed).astype(jnp.bfloat16))


def solution(mesh):
    placed = (
        P("ep", "tp"),
        P("ep", "tp"),
        P(None, "tp"),
        P("tp"),
        P("tp", None),
        P("ep", None),
        P(),
        P("ep", None),
        P("ep", None),
        P("ep", None, "tp"),
        P("ep", None, "tp"),
        P("ep", "tp", None),
        P(),
        P(),
        P(None, "tp"),
    )
    return jax.shard_map(
        local, mesh=mesh, in_specs=placed, out_specs=(P("ep", "tp"), P("ep", "tp")), check_vma=False
    )
```
